32 devices in a mesh: ep: 8 (over z, y), tp: 4 (over x, core).
Axes of the slice: x: 2, y: 2, z: 4, core: 2. Of those that a mesh axis runs over, the one named last changes fastest.
Arguments:
- tokens: bfloat16 [128, 2048], P('ep'), may hold values from -60 to 60
- mixer_gain: float32 [2048], replicated, may hold values from 0.1 to 1.9
- query_weight: bfloat16 [2048, 2048], P('ep', 'tp'), may hold values from -0.125 to 0.125
- key_weight: bfloat16 [2048, 2048], P('ep', 'tp'), may hold values from -0.125 to 0.125
- value_weight: bfloat16 [2048, 2048], P('ep', 'tp'), may hold values from -0.125 to 0.125
- outgate_weight: bfloat16 [2048, 2048], P('ep', 'tp'), may hold values from -0.125 to 0.125
- igate_weight: bfloat16 [4, 2048], P('tp'), may hold values from -0.125 to 0.125
- fgate_weight: bfloat16 [4, 2048], P('tp'), may hold values from -0.125 to 0.125
- memory: float32 [128, 4, 512, 512], P('ep', 'tp'), may hold values from -6 to 6
- stabilizer: float32 [128, 4], P('ep', 'tp'), may hold values from -6 to 6
- head_gain: float32 [2048], P('tp'), may hold values from 0.1 to 1.9
- down_weight: bfloat16 [2048, 2048], P(None, 'ep'), may hold values from -1 to 1
- mixed_gain: float32 [2048], P('ep'), may hold values from 0.1 to 1.9
- expert_gain: float32 [2048], P('ep'), may hold values from 0.1 to 1.9
- routes: int32 [128, 4], replicated, may hold values from 0 to 7, all different within a row; in each aligned block of 16 rows (0 to 15, 16 to 31, ...) at most 16 rows name the same one
- route_weights: float32 [128, 4], replicated, may hold values from 0.1 to 1
- gate_proj: bfloat16 [8, 2048, 2048], P('ep', None, 'tp'), may hold values from -0.5 to 0.5
- up_proj: bfloat16 [8, 2048, 2048], P('ep', None, 'tp'), may hold values from -0.5 to 0.5
- expert_down: bfloat16 [8, 2048, 2048], P('ep', 'tp'), may hold values from -1 to 1
- output_gain: float32 [2048], P('tp'), may hold values from 0.1 to 1.9
Outputs:
- layer_out: bfloat16 [128, 2048], P('ep', 'tp')
The draws below stay inside these ranges and needn't reach their ends.
Inputs may be any that keep to these rules, and one draw needn't show every extreme that they name: `routes`: each row names 4 different experts; within the rows of one device (16 rows) no expert is named more than 16 times, a bound that some block reaches.
All inputs are finite; a program needn't handle non-finite values.
Results may differ from the reference program's by a relative error of at most 0.0095.
Values may be sent and summed in bfloat16 or wider, within the bound.
A program may use at most 128 MiB of HBM per device.

```python
import math
import jax
import jax.numpy as jnp
import numpy as np
from jax import lax

D = 2048
HEADS = 4
DH = 512
DE = 2048
TOP_K = 4
SEQ_DEV = 16
TOKENS = 128
EXPERTS = 8
CAP = 16
N_EP = 8


def column_ramp(key, width, spread):
    rough = jax.random.uniform(key, (width,), jnp.float32, -0.3, 0.3)
    return jnp.exp(jnp.linspace(-spread, spread, width) + rough)


def draw_tokens(key, part):
    base = jax.random.normal(jax.random.fold_in(key, 11), (TOKENS, D), jnp.float32)
    row_scale = jnp.exp(jax.random.uniform(jax.random.fold_in(key, 12), (TOKENS, 1), jnp.float32, jnp.log(0.4), jnp.log(4.0)))
    ramp = column_ramp(jax.random.fold_in(key, 14), D, 0.55)
    values = base * row_scale * ramp[None, :]
    return jnp.clip(values, -60.0, 60.0).astype(jnp.bfloat16)


def draw_down_weight(key, part):
    base = jax.random.normal(jax.random.fold_in(key, 21), (HEADS * DH, D), jnp.float32) / jnp.sqrt(HEADS * DH * 1.0)
    ramp = column_ramp(jax.random.fold_in(key, 22), D, 0.55)
    return jnp.clip(base * ramp[None, :], -1.0, 1.0).astype(jnp.bfloat16)


def draw_expert_down(key, part):
    base = jax.random.normal(jax.random.fold_in(key, 31), (EXPERTS, DE, D), jnp.float32) / jnp.sqrt(DE * 1.0)
    ramp = column_ramp(jax.random.fold_in(key, 32), D, 0.55)
    return jnp.clip(base * ramp[None, None, :], -1.0, 1.0).astype(jnp.bfloat16)


def level_of(own_key, shape, shards, low, high):
    def one(dim, parts):
        draws = jax.random.uniform(jax.random.fold_in(jax.random.fold_in(own_key, 6), dim), (parts,), jnp.float32, low / len(shards), high / len(shards))
        return jnp.repeat(jnp.exp(draws), shape[dim] // parts).reshape((-1,) + (1,) * (len(shape) - dim - 1))

    loudness = one(*shards[0])
    for cut in shards[1:]:
        loudness = loudness * one(*cut)
    return loudness


def assign_block(stream_key, own, number, rows, amount, top, bound, skew):
    order = jax.random.permutation(stream_key, amount)
    crowded, usual = load_shares(amount, rows * top, bound, skew, True), load_shares(amount, rows * top, bound, skew, False)
    places = jnp.arange(amount)

    def named(lengths, rotation):
        used = int((lengths > 0).sum())
        fixed = max(1, used // 4)
        passed = fixed + (places - fixed + rotation * (used - fixed)) % max(1, amount - fixed)
        return jnp.zeros((amount,), jnp.int32).at[order[jnp.where(places < fixed, places, passed)]].set(jnp.asarray(lengths, jnp.int32))

    lengths = jnp.where(number % 4 == 0, named(crowded, number // 4), named(usual, number - number // 4 - 1))
    mixed = jax.random.permutation(jax.random.fold_in(own, 3), amount)
    donor, sink = mixed[0:amount // 2 * 2:2], mixed[1:amount // 2 * 2:2]
    slack = jnp.minimum(lengths[donor] - 1, bound - lengths[sink]) // 2
    slack = jnp.where((donor == order[0]) | (sink == order[0]) | (lengths[sink] == 0), 0, jnp.maximum(slack, 0))
    passed = jax.random.randint(jax.random.fold_in(own, 4), (amount // 2,), 0, 1 << 20) % (slack + 1)
    lengths = lengths.at[donor].add(-passed).at[sink].add(passed)
    members = jnp.searchsorted(jnp.cumsum(lengths), jnp.arange(rows * top), side="right").astype(jnp.int32)
    table = members.reshape(top, rows).T
    table = table[jax.random.permutation(jax.random.fold_in(own, 1), rows)]
    rotation = jax.random.randint(jax.random.fold_in(own, 2), (rows, 1), 0, top)
    return jnp.take_along_axis(table, (jnp.arange(top)[None, :] + rotation) % top, axis=1)


def load_shares(count, total, most, lean, full):
    loads = [(1 << 20) // math.isqrt(standing ** lean) + 1 for standing in range(1, count + 1)]
    largest = most if full else min(most, max(-(-total // count), total * loads[0] // sum(loads)))
    least = 1 if total - largest >= count - 1 else 0
    given, surplus = [largest] + [least] * (count - 1), total - largest - least * (count - 1)
    while surplus > 0:
        free = [i for i in range(1, count) if given[i] < largest] or [i for i in range(1, count) if given[i] < most]
        mass, budget = sum([loads[i] for i in free]), surplus
        for i in free:
            extra = min(most - given[i], max(1, budget * loads[i] // mass), surplus)
            given[i] = given[i] + extra
            surplus = surplus - extra
    return np.array(given)


def centred(key, shape, scale, reach, cuts=(), held_as=jnp.bfloat16):
    loudness = level_of(key, shape, cuts, -0.22, 0.18) if cuts else 1.0
    drawn = jax.random.normal(key, shape, jnp.float32) * scale * loudness
    return jnp.minimum(jnp.maximum(drawn, -reach), reach).astype(held_as)


def setup_inputs(seed: int = 0) -> dict:
    streams_of = jax.random.split(jax.random.key(seed), 21)
    tokens = draw_tokens(jax.random.fold_in(streams_of[20], 71), 0)
    mixer_gain = jnp.clip(1.0 + 0.18 * jax.random.normal(streams_of[1], (D,), jnp.float32), 0.1, 1.9)
    query_weight = centred(streams_of[2], (D, HEADS * DH), D ** -0.5, 0.125, ((0, 8), (1, 4)))
    key_weight = centred(streams_of[3], (D, HEADS * DH), D ** -0.5, 0.125, ((0, 8), (1, 4)))
    value_weight = centred(streams_of[4], (D, HEADS * DH), D ** -0.5, 0.125, ((0, 8), (1, 4)))
    outgate_weight = centred(streams_of[5], (D, HEADS * DH), D ** -0.5, 0.125, ((0, 8), (1, 4)))
    igate_weight = centred(streams_of[6], (HEADS, D), D ** -0.5, 0.125, ((0, 4),))
    fgate_weight = centred(streams_of[7], (HEADS, D), D ** -0.5, 0.125, ((0, 4),))
    memory = centred(streams_of[8], (TOKENS, HEADS, DH, DH), 1.0, 6.0, ((0, 8), (1, 4)), jnp.float32)
    stabilizer = centred(streams_of[9], (TOKENS, HEADS), 1.5, 6.0, ((0, 8), (1, 4)), jnp.float32)
    head_gain = jnp.clip(1.0 + 0.18 * jax.random.normal(streams_of[10], (HEADS * DH,), jnp.float32), 0.1, 1.9)
    down_weight = draw_down_weight(jax.random.fold_in(streams_of[20], 71), 0)
    mixed_gain = jnp.clip(1.0 + 0.18 * jax.random.normal(streams_of[12], (D,), jnp.float32), 0.1, 1.9)
    expert_gain = jnp.clip(1.0 + 0.18 * jax.random.normal(streams_of[13], (D,), jnp.float32), 0.1, 1.9)
    routes_keys = jax.random.split(jax.random.fold_in(streams_of[14], 1), TOKENS // SEQ_DEV)
    routes_turns = jax.random.permutation(jax.random.fold_in(streams_of[14], 3), TOKENS // SEQ_DEV)
    routes = jax.vmap(lambda own, number: assign_block(jax.random.fold_in(streams_of[14], 2), own, number, SEQ_DEV, EXPERTS, TOP_K, CAP, 2))(routes_keys, routes_turns).reshape((TOKENS, TOP_K))
    route_weights = jnp.clip(jax.random.uniform(streams_of[15], (TOKENS, TOP_K), jnp.float32, 0.1, 1.0), 0.1, 1.0)
    gate_proj = centred(streams_of[16], (EXPERTS, D, DE), (D // 16) ** -0.5, 0.5, ((0, 8), (2, 4)))
    up_proj = centred(streams_of[17], (EXPERTS, D, DE), (D // 16) ** -0.5, 0.5, ((0, 8), (2, 4)))
    expert_down = draw_expert_down(jax.random.fold_in(streams_of[20], 71), 0)
    output_gain = jnp.clip(1.0 + 0.18 * jax.random.normal(streams_of[19], (D,), jnp.float32), 0.1, 1.9)
    return dict(tokens=tokens, mixer_gain=mixer_gain, query_weight=query_weight, key_weight=key_weight, value_weight=value_weight, outgate_weight=outgate_weight, igate_weight=igate_weight, fgate_weight=fgate_weight, memory=memory, stabilizer=stabilizer, head_gain=head_gain, down_weight=down_weight, mixed_gain=mixed_gain, expert_gain=expert_gain, routes=routes, route_weights=route_weights, gate_proj=gate_proj, up_proj=up_proj, expert_down=expert_down, output_gain=output_gain)


NORM_EPS = 1e-06
CLAMP_LIMIT = 7.0
SIGMOID_SCALE = 1.702

def rms_scale(values):
    return lax.rsqrt(lax.optimization_barrier(jnp.mean(values * values, axis=-1, keepdims=True)) + NORM_EPS)

def slot_tables(routes, groups, experts, capacity):
    token_total, top_count = routes.shape
    per_group = token_total // groups
    flat_routes = routes.reshape(groups, per_group * top_count)
    onehot = (flat_routes[:, :, None] == jnp.arange(experts, dtype=jnp.int32)[None, None, :]).astype(jnp.int32)
    before = jnp.cumsum(onehot, axis=1) - onehot
    slot_index = lax.optimization_barrier(jnp.sum(before * onehot, axis=2))
    group_ids = jnp.arange(groups, dtype=jnp.int32)[:, None]
    destination = ((flat_routes * groups + group_ids) * capacity + slot_index).reshape(token_total, top_count)
    owner_token = jnp.arange(token_total * top_count, dtype=jnp.int32) // top_count
    slot_token = jnp.full((experts * groups * capacity,), token_total, jnp.int32).at[destination.reshape(-1)].set(owner_token)
    return (destination, slot_token)

def read_memory(projected, log_input, log_forget, memory, stabilizer, head_gain):
    row_total, head_count, head_size = (memory.shape[0], memory.shape[1], memory.shape[3])
    query_scaled = projected[:, 0] * head_size ** (-0.5)
    key_rows = projected[:, 1]
    value_rows = projected[:, 2]
    outgate_rows = projected[:, 3]
    peak_log = jnp.maximum(log_forget + stabilizer, log_input)
    within = jnp.exp(log_input - peak_log)
    carried = jnp.exp(log_forget + stabilizer - peak_log)
    scores = lax.optimization_barrier(jnp.sum(query_scaled * key_rows, axis=-1)) * within
    state_read = jnp.einsum('nhd,nhde->nhe', query_scaled, memory, precision=lax.Precision.HIGHEST)
    read_value = scores[..., None] * value_rows + carried[..., None] * state_read
    head_mean = lax.optimization_barrier(jnp.mean(read_value, axis=-1, keepdims=True))
    centered = read_value - head_mean
    head_var = lax.optimization_barrier(jnp.mean(centered * centered, axis=-1, keepdims=True))
    normalized = centered * lax.rsqrt(head_var + NORM_EPS)
    gained = normalized * head_gain.reshape(head_count, head_size) * jax.nn.sigmoid(outgate_rows)
    return gained.reshape(row_total, head_count * head_size).astype(jnp.bfloat16)

def apply_expert(arguments):
    row_block, gate_matrix, up_matrix, down_matrix = arguments
    gate_pre = jnp.minimum(jnp.dot(row_block, gate_matrix, preferred_element_type=jnp.float32), CLAMP_LIMIT)
    up_pre = jnp.clip(jnp.dot(row_block, up_matrix, preferred_element_type=jnp.float32), -CLAMP_LIMIT, CLAMP_LIMIT)
    activation = ((up_pre + 1.0) * gate_pre * jax.nn.sigmoid(SIGMOID_SCALE * gate_pre)).astype(jnp.bfloat16)
    return jnp.dot(activation, down_matrix, preferred_element_type=jnp.float32)

def reference(tokens, mixer_gain, query_weight, key_weight, value_weight, outgate_weight, igate_weight, fgate_weight, memory, stabilizer, head_gain, down_weight, mixed_gain, expert_gain, routes, route_weights, gate_proj, up_proj, expert_down, output_gain):
    tokens_float = tokens.astype(jnp.float32)
    normed = (tokens_float * rms_scale(tokens_float) * mixer_gain).astype(jnp.bfloat16)
    projected = jnp.concatenate([jnp.dot(normed, matrix, preferred_element_type=jnp.float32) for matrix in (query_weight, key_weight, value_weight, outgate_weight)], axis=1).astype(jnp.bfloat16)
    projected = lax.optimization_barrier(projected).astype(jnp.float32).reshape(TOKENS, 4, HEADS, DH)
    log_input = jnp.dot(normed, igate_weight.T, preferred_element_type=jnp.float32)
    log_forget = jax.nn.log_sigmoid(jnp.dot(normed, fgate_weight.T, preferred_element_type=jnp.float32))
    gated_heads = read_memory(projected, log_input, log_forget, memory, stabilizer, head_gain)
    mixed_rows = jnp.dot(gated_heads, down_weight, preferred_element_type=jnp.float32)
    residual_float = tokens_float + mixed_rows * rms_scale(mixed_rows) * mixed_gain
    residual = residual_float.astype(jnp.bfloat16)
    expert_in = (residual_float * rms_scale(residual_float) * expert_gain).astype(jnp.bfloat16)
    destination, slot_token = slot_tables(routes, N_EP, EXPERTS, CAP)
    padded_in = jnp.concatenate([expert_in, jnp.zeros((1, D), jnp.bfloat16)], axis=0)
    expert_inputs = padded_in[slot_token].reshape(EXPERTS, N_EP * CAP, D)
    expert_out = lax.map(apply_expert, (expert_inputs, gate_proj, up_proj, expert_down))
    picked = expert_out.reshape(EXPERTS * N_EP * CAP, D)[destination]
    combined = lax.optimization_barrier(jnp.sum(picked * route_weights[..., None], axis=1))
    final_rows = residual.astype(jnp.float32) + combined * rms_scale(combined) * output_gain
    return final_rows.astype(jnp.bfloat16)
```

```python
import functools

import jax
import jax.numpy as jnp
from jax import lax
from jax.experimental import pallas as pl
from jax.experimental.pallas import tpu as pltpu
from jax.sharding import PartitionSpec as P

NORM_EPS = 1e-06
CLAMP_LIMIT = 7.0
SIGMOID_SCALE = 1.702
F32 = jnp.float32
BF16 = jnp.bfloat16


def rms_scale(values):
    return lax.rsqrt(jnp.mean(values * values, axis=-1, keepdims=True) + NORM_EPS)


def log_sigmoid(values):
    return jnp.minimum(values, 0.0) - jnp.log(1.0 + jnp.exp(-jnp.abs(values)))


def layer_kernel(n_ep, n_tp, *refs):
    (
        tokens, mixer_gain, igate, fgate, stabilizer, head_gain, mixed_gain, expert_gain,
        routes, route_weights, output_gain,
        query_weight, key_weight, value_weight, outgate_weight, memory, down_weight,
        gate_proj, up_proj, expert_down,
        out,
        w4, memv, downv, gatev, upv, edownv,
        xsend, xrecv, tok_all, gains, qk_send, qk_recv, vo_send, vo_recv, gsend, grecv, mixed_all, resid, expert_in,
        esend, erecv, ssend, srecv, squares, read_rows,
        lsem, x_s, x_r, t_s, t_r, n_s, n_r, k_s, k_r, p_s, p_r, tf_s, tf_r, g_s, g_r, m_s, m_r, f_s, f_r,
        e_s, e_r, c_s, c_r, q_s, q_r,
    ) = refs
    me_e = lax.axis_index("ep")
    me_t = lax.axis_index("tp")
    rows, width = tokens.shape
    heads, head_size = memory.shape[1], memory.shape[3]
    head_width = heads * head_size
    slice_width = width // n_ep
    tp_width = width // n_tp
    ratio = n_ep // n_tp
    total = n_ep * rows
    quarter = ratio * rows
    experts = gate_proj.shape[0]

    def remote(src, dst, ssem, rsem, ep, tp):
        return pltpu.make_async_remote_copy(
            src_ref=src, dst_ref=dst, send_sem=ssem, recv_sem=rsem,
            device_id=(ep, tp), device_id_type=pl.DeviceIdType.MESH,
        )

    def loop(low, high, step):
        def run(i, carry):
            step(i)
            return carry

        lax.fori_loop(low, high, run, 0)

    def ep_at(i):
        return lax.rem(me_e + i, n_ep)

    def ep_back(i):
        return lax.rem(me_e - i + n_ep, n_ep)

    def tp_at(i):
        return lax.rem(me_t + i, n_tp)

    local = []

    def fetch(src, dst):
        copy = pltpu.make_async_copy(src, dst, lsem.at[len(local)])
        copy.start()
        local.append(copy)
        return copy

    weight_copies = [
        fetch(ref, w4.at[i])
        for i, ref in enumerate((query_weight, key_weight, value_weight, outgate_weight))
    ]
    chunk = rows // 4
    memory_copies = [
        fetch(memory.at[pl.ds(i * chunk, chunk)], memv.at[pl.ds(i * chunk, chunk)])
        for i in range(4)
    ]
    down_copy = fetch(down_weight, downv)
    gate_copy = fetch(gate_proj, gatev)
    up_copy = fetch(up_proj, upv)
    edown_copy = fetch(expert_down, edownv)

    barrier = pltpu.get_barrier_semaphore()
    devices = n_ep * n_tp
    flat = me_e * n_tp + me_t

    def greet(i):
        other = lax.rem(flat + i, devices)
        pl.semaphore_signal(
            barrier, inc=1, device_id=(lax.div(other, n_tp), lax.rem(other, n_tp)),
            device_id_type=pl.DeviceIdType.MESH,
        )

    loop(1, devices, greet)

    tokens_float = tokens[...].astype(F32)
    normed = (tokens_float * rms_scale(tokens_float) * mixer_gain[...]).astype(BF16)
    for j in range(n_ep):
        xsend[j] = normed[:, j * slice_width : (j + 1) * slice_width]
    xrecv[me_e] = xsend[me_e]
    own_rows = pl.ds(pl.multiple_of(me_e * rows, rows), rows)
    tok_all[me_t, own_rows, :] = tokens[:, pl.ds(pl.multiple_of(me_t * tp_width, tp_width), tp_width)]
    gain_row = lax.broadcasted_iota(jnp.int32, (8, slice_width), 0)
    gains[me_e] = jnp.where(gain_row == 0, mixed_gain[...], expert_gain[...])
    pl.semaphore_wait(barrier, devices - 1)

    def x_copy(i):
        dst = ep_at(i)
        return remote(xsend.at[dst], xrecv.at[me_e], x_s.at[dst], x_r.at[me_e], dst, me_t)

    def t_copy(i):
        dst = ep_at(i)
        block = tok_all.at[me_t, own_rows]
        return remote(block, block, t_s.at[dst], t_r.at[me_e], dst, me_t)

    def n_copy(i):
        dst = ep_at(i)
        return remote(gains.at[me_e], gains.at[me_e], n_s.at[dst], n_r.at[me_e], dst, me_t)

    loop(1, n_ep, lambda i: x_copy(i).start())

    normed_float = normed.astype(F32)
    log_input = [
        jnp.sum(normed_float * igate[h : h + 1, :].astype(F32), axis=-1, keepdims=True)
        for h in range(heads)
    ]
    log_forget = [
        log_sigmoid(jnp.sum(normed_float * fgate[h : h + 1, :].astype(F32), axis=-1, keepdims=True))
        for h in range(heads)
    ]

    for copy in weight_copies:
        copy.wait()

    def x_wait(i):
        src = ep_back(i)
        remote(xrecv.at[src], xrecv.at[src], x_s.at[src], x_r.at[src], src, me_t).wait_recv()

    loop(1, n_ep, x_wait)
    features = jnp.concatenate([xrecv[j] for j in range(n_ep)], axis=0)

    def k_copy(j, i):
        dst = ep_at(i)
        return remote(
            qk_send.at[j, dst], qk_recv.at[j, me_e], k_s.at[j, dst], k_r.at[j, me_e], dst, me_t
        )

    def p_copy(i):
        dst = ep_at(i)
        return remote(vo_send.at[dst], vo_recv.at[me_e], p_s.at[dst], p_r.at[me_e], dst, me_t)

    for j in range(2):
        part = jnp.dot(features, w4[j], preferred_element_type=F32)
        qk_send[j] = part.reshape(n_ep, rows, head_width)
        loop(1, n_ep, lambda i: k_copy(j, i).start())
        qk_recv[j, me_e] = qk_send[j, me_e]
    for j in range(2):
        part = jnp.dot(features, w4[2 + j], preferred_element_type=F32).astype(BF16)
        vo_send[:, :, j * head_width : (j + 1) * head_width] = part.reshape(n_ep, rows, head_width)
    loop(1, n_ep, lambda i: p_copy(i).start())
    vo_recv[me_e] = vo_send[me_e]
    loop(1, n_ep, lambda i: t_copy(i).start())
    loop(1, n_ep, lambda i: n_copy(i).start())

    def k_wait(j, i):
        src = ep_back(i)
        block = qk_recv.at[j, src]
        remote(block, block, k_s.at[j, src], k_r.at[j, src], src, me_t).wait_recv()

    def p_wait(i):
        src = ep_back(i)
        remote(vo_recv.at[src], vo_recv.at[src], p_s.at[src], p_r.at[src], src, me_t).wait_recv()

    def total_of(ref, *lead):
        value = ref[(*lead, 0)].astype(F32)
        for j in range(1, n_ep):
            value = value + ref[(*lead, j)].astype(F32)
        return value.astype(BF16).astype(F32)

    loop(1, n_ep, lambda i: k_wait(0, i))
    all_query = total_of(qk_recv, 0) * head_size ** (-0.5)

    for copy in memory_copies:
        copy.wait()
    for h in range(heads):
        query_columns = all_query[:, h * head_size : (h + 1) * head_size].T
        for n in range(rows):
            column = query_columns[:, n : n + 1]
            step = 64
            acc = jnp.zeros((8, head_size), F32)
            for d in range(0, head_size, step):
                prod = column[d : d + step, :] * memv[n, h, d : d + step, :]
                acc = acc + jnp.sum(prod.reshape(step // 8, 8, head_size), axis=0)
            read_rows[h, n : n + 1, :] = jnp.sum(acc, axis=0, keepdims=True)
    loop(1, n_ep, lambda i: k_wait(1, i))
    all_key = total_of(qk_recv, 1)
    loop(1, n_ep, p_wait)
    all_gated = total_of(vo_recv)
    for h in range(heads):
        head = slice(h * head_size, (h + 1) * head_size)
        query, key = all_query[:, head], all_key[:, head]
        value = all_gated[:, head]
        outgate = all_gated[:, head_width + h * head_size : head_width + (h + 1) * head_size]
        carried_log = log_forget[h] + stabilizer[:, h : h + 1]
        peak = jnp.maximum(carried_log, log_input[h])
        within = jnp.exp(log_input[h] - peak)
        carried = jnp.exp(carried_log - peak)
        score = jnp.sum(query * key, axis=-1, keepdims=True) * within
        read = score * value + carried * read_rows[h]
        centered = read - jnp.mean(read, axis=-1, keepdims=True)
        variance = jnp.mean(centered * centered, axis=-1, keepdims=True)
        gained = centered * lax.rsqrt(variance + NORM_EPS)
        gained = gained * head_gain[:, h * head_size : (h + 1) * head_size]
        gained = gained * jax.nn.sigmoid(outgate)
        gsend[:, h * head_size : (h + 1) * head_size] = gained.astype(BF16)

    group = lax.div(me_e, ratio)
    place = lax.rem(me_e, ratio)
    place_rows = pl.ds(pl.multiple_of(place * rows, rows), rows)
    home = group == me_t

    def g_copy(dst):
        return remote(
            gsend, grecv.at[me_t, place_rows], g_s.at[dst], g_r.at[place * n_tp + me_t], dst, group
        )

    @pl.when(home)
    def _():
        grecv[me_t, place_rows, :] = gsend[...]

    @pl.when(jnp.logical_not(home))
    def _():
        g_copy(me_e).start()

    loop(1, n_ep, lambda i: g_copy(ep_at(i)).start())

    def t_wait(i):
        src = ep_back(i)
        block = tok_all.at[me_t, pl.ds(pl.multiple_of(src * rows, rows), rows)]
        remote(block, block, t_s.at[src], t_r.at[src], src, me_t).wait_recv()
        remote(gains.at[src], gains.at[src], n_s.at[src], n_r.at[src], src, me_t).wait_recv()

    loop(1, n_ep, t_wait)

    def tf_copy(i):
        dst = tp_at(i)
        return remote(tok_all.at[me_t], tok_all.at[me_t], tf_s.at[dst], tf_r.at[me_t], me_e, dst)

    loop(1, n_tp, lambda i: tf_copy(i).start())

    def g_wait(k):
        src_place, src_t = lax.div(k, n_tp), lax.rem(k, n_tp)
        src_e = me_t * ratio + src_place

        @pl.when(jnp.logical_or(src_e != me_e, src_t != me_t))
        def _():
            block = grecv.at[src_t, pl.ds(pl.multiple_of(src_place * rows, rows), rows)]
            remote(block, block, g_s.at[0], g_r.at[k], src_e, src_t).wait_recv()

    down_copy.wait()
    loop(0, ratio * n_tp, g_wait)
    mixed = jnp.dot(grecv[0], downv[0:head_width, :], preferred_element_type=F32)
    for s in range(1, n_tp):
        mixed = mixed + jnp.dot(
            grecv[s], downv[s * head_width : (s + 1) * head_width, :], preferred_element_type=F32
        )

    def token_rows(t):
        return pl.ds(pl.multiple_of(t * quarter, quarter), quarter)

    mixed_all[me_e, token_rows(me_t), :] = mixed.astype(BF16)

    def m_copy(i):
        dst = ep_at(i)
        block = mixed_all.at[me_e, token_rows(me_t)]
        return remote(block, block, m_s.at[dst], m_r.at[me_e], dst, me_t)

    def f_copy(src, i):
        dst = tp_at(i)
        block = mixed_all.at[src, token_rows(me_t)]
        return remote(block, block, f_s.at[src, dst], f_r.at[src, me_t], me_e, dst)

    loop(1, n_ep, lambda i: m_copy(i).start())
    loop(1, n_tp, lambda i: f_copy(me_e, i).start())

    def m_pass(i):
        src = ep_back(i)
        block = mixed_all.at[src, token_rows(me_t)]
        remote(block, block, m_s.at[src], m_r.at[src], src, me_t).wait_recv()
        loop(1, n_tp, lambda k: f_copy(src, k).start())

    loop(1, n_ep, m_pass)

    def tf_wait(i):
        src = tp_at(i)
        remote(tok_all.at[src], tok_all.at[src], tf_s.at[src], tf_r.at[src], me_e, src).wait_recv()

    loop(1, n_tp, tf_wait)

    def f_wait(i):
        src = ep_back(i)
        for k in range(1, n_tp):
            t = tp_at(k)
            block = mixed_all.at[src, token_rows(t)]
            remote(block, block, f_s.at[src, t], f_r.at[src, t], me_e, t).wait_recv()

    loop(0, n_ep, f_wait)

    mixed_squares = jnp.zeros((total, 1), F32)
    for j in range(n_ep):
        block = mixed_all[j].astype(F32)
        mixed_squares = mixed_squares + jnp.sum(block * block, axis=-1, keepdims=True)
    mixed_scale = lax.rsqrt(mixed_squares / width + NORM_EPS)
    residual_squares = jnp.zeros((total, 1), F32)
    for j in range(n_ep):
        start = j * slice_width
        owner, offset = start // tp_width, start % tp_width
        block = tok_all[owner, :, offset : offset + slice_width].astype(F32)
        block = block + mixed_all[j].astype(F32) * mixed_scale * gains[j, 0:1, :]
        resid[:, start : start + slice_width] = block
        residual_squares = residual_squares + jnp.sum(block * block, axis=-1, keepdims=True)
    residual_scale = lax.rsqrt(residual_squares / width + NORM_EPS)
    for j in range(n_ep):
        start = j * slice_width
        block = resid[:, start : start + slice_width] * residual_scale * gains[j, 1:2, :]
        expert_in[:, start : start + slice_width] = block.astype(BF16)

    gate_copy.wait()
    up_copy.wait()
    acts, weights = [], []
    for l in range(experts):
        gate = jnp.dot(expert_in[...], gatev[l], preferred_element_type=F32)
        up = jnp.dot(expert_in[...], upv[l], preferred_element_type=F32)
        gate = jnp.minimum(gate, CLAMP_LIMIT)
        up = jnp.clip(up, -CLAMP_LIMIT, CLAMP_LIMIT)
        acts.append(((up + 1.0) * gate * jax.nn.sigmoid(SIGMOID_SCALE * gate)).astype(BF16))
        hit = routes[...] == me_e * experts + l
        weights.append(jnp.sum(jnp.where(hit, route_weights[...], 0.0), axis=-1, keepdims=True))
    edown_copy.wait()

    def expert_part(t):
        columns = pl.ds(pl.multiple_of(t * tp_width, tp_width), tp_width)
        value = None
        for l in range(experts):
            one = jnp.dot(acts[l], edownv[l, :, columns], preferred_element_type=F32) * weights[l]
            value = one if value is None else value + one
        return value

    def e_copy(i):
        dst = tp_at(i)
        return remote(esend.at[i], erecv.at[me_t], e_s.at[i], e_r.at[me_t], me_e, dst)

    for i in range(1, n_tp):
        esend[i] = expert_part(tp_at(i)).astype(BF16)
        e_copy(i).start()
    combined_part = expert_part(me_t)
    for i in range(1, n_tp):
        src = tp_at(i)
        remote(erecv.at[src], erecv.at[src], e_s.at[0], e_r.at[src], me_e, src).wait_recv()
        combined_part = combined_part + erecv[src].astype(F32)
    ssend[...] = combined_part.astype(BF16).reshape(n_ep, rows, tp_width)

    def c_copy(i):
        dst = ep_at(i)
        return remote(ssend.at[dst], srecv.at[me_e], c_s.at[dst], c_r.at[me_e], dst, me_t)

    loop(1, n_ep, lambda i: c_copy(i).start())
    srecv[me_e] = ssend[me_e]

    def c_wait(i):
        src = ep_back(i)
        remote(srecv.at[src], srecv.at[src], c_s.at[src], c_r.at[src], src, me_t).wait_recv()

    loop(1, n_ep, c_wait)
    combined = srecv[0].astype(F32)
    for j in range(1, n_ep):
        combined = combined + srecv[j].astype(F32)
    own_squares = jnp.sum(combined * combined, axis=-1, keepdims=True)
    squares[me_t] = jnp.broadcast_to(own_squares, squares.shape[1:])

    def q_copy(i):
        dst = tp_at(i)
        return remote(squares.at[me_t], squares.at[me_t], q_s.at[dst], q_r.at[me_t], me_e, dst)

    loop(1, n_tp, lambda i: q_copy(i).start())
    own_columns = pl.ds(pl.multiple_of(me_t * tp_width, tp_width), tp_width)
    residual = resid[own_rows, own_columns].astype(BF16).astype(F32)

    def q_wait(i):
        src = tp_at(i)
        remote(squares.at[src], squares.at[src], q_s.at[src], q_r.at[src], me_e, src).wait_recv()

    loop(1, n_tp, q_wait)
    all_squares = squares[0]
    for t in range(1, n_tp):
        all_squares = all_squares + squares[t]
    scale = lax.rsqrt(all_squares[:, 0:1] / width + NORM_EPS)
    out[...] = (residual + combined * scale * output_gain[...]).astype(BF16)

    def ep_sends(i):
        x_copy(i).wait_send()
        t_copy(i).wait_send()
        n_copy(i).wait_send()
        k_copy(0, i).wait_send()
        k_copy(1, i).wait_send()
        p_copy(i).wait_send()
        g_copy(ep_at(i)).wait_send()
        m_copy(i).wait_send()
        c_copy(i).wait_send()

    loop(1, n_ep, ep_sends)

    @pl.when(jnp.logical_not(home))
    def _():
        g_copy(me_e).wait_send()

    def tp_sends(i):
        tf_copy(i).wait_send()
        e_copy(i).wait_send()
        q_copy(i).wait_send()
        loop(0, n_ep, lambda j: f_copy(ep_at(j), i).wait_send())

    loop(1, n_tp, tp_sends)


def shards(
    n_ep, n_tp, tokens, mixer_gain, query_weight, key_weight, value_weight, outgate_weight,
    igate_weight, fgate_weight, memory, stabilizer, head_gain, down_weight, mixed_gain,
    expert_gain, routes, route_weights, gate_proj, up_proj, expert_down, output_gain,
):
    rows, width = tokens.shape
    heads, head_size = memory.shape[1], memory.shape[3]
    head_width = heads * head_size
    slice_width = width // n_ep
    tp_width = width // n_tp
    total = n_ep * rows
    quarter = total // n_tp
    vmem = pltpu.VMEM
    dma = pltpu.SemaphoreType.DMA
    small = (
        tokens, mixer_gain.reshape(1, -1), igate_weight, fgate_weight, stabilizer,
        head_gain.reshape(1, -1), mixed_gain.reshape(1, -1), expert_gain.reshape(1, -1),
        routes, route_weights, output_gain.reshape(1, -1),
    )
    large = (
        query_weight, key_weight, value_weight, outgate_weight, memory, down_weight,
        gate_proj, up_proj, expert_down,
    )
    scratch = [
        vmem((4,) + query_weight.shape, BF16),
        vmem(memory.shape, F32),
        vmem(down_weight.shape, BF16),
        vmem(gate_proj.shape, BF16),
        vmem(up_proj.shape, BF16),
        vmem(expert_down.shape, BF16),
        vmem((n_ep, rows, slice_width), BF16),
        vmem((n_ep, rows, slice_width), BF16),
        vmem((n_tp, total, tp_width), BF16),
        vmem((n_ep, 8, slice_width), F32),
        vmem((2, n_ep, rows, head_width), F32),
        vmem((2, n_ep, rows, head_width), F32),
        vmem((n_ep, rows, 2 * head_width), BF16),
        vmem((n_ep, rows, 2 * head_width), BF16),
        vmem((rows, head_width), BF16),
        vmem((n_tp, quarter, head_width), BF16),
        vmem((n_ep, total, slice_width), BF16),
        vmem((total, width), F32),
        vmem((total, width), BF16),
        vmem((n_tp, total, tp_width), BF16),
        vmem((n_tp, total, tp_width), BF16),
        vmem((n_ep, rows, tp_width), BF16),
        vmem((n_ep, rows, tp_width), BF16),
        vmem((n_tp, rows, 128), F32),
        vmem((heads, rows, head_size), F32),
        dma((12,)),
        dma((n_ep,)), dma((n_ep,)),
        dma((n_ep,)), dma((n_ep,)),
        dma((n_ep,)), dma((n_ep,)),
        dma((2, n_ep)), dma((2, n_ep)),
        dma((n_ep,)), dma((n_ep,)),
        dma((n_tp,)), dma((n_tp,)),
        dma((n_ep,)), dma((n_ep,)),
        dma((n_ep,)), dma((n_ep,)),
        dma((n_ep, n_tp)), dma((n_ep, n_tp)),
        dma((n_tp,)), dma((n_tp,)),
        dma((n_ep,)), dma((n_ep,)),
        dma((n_tp,)), dma((n_tp,)),
    ]
    return pl.pallas_call(
        functools.partial(layer_kernel, n_ep, n_tp),
        out_shape=jax.ShapeDtypeStruct((rows, tp_width), BF16),
        in_specs=[pl.BlockSpec(memory_space=vmem)] * len(small)
        + [pl.BlockSpec(memory_space=pl.ANY)] * len(large),
        out_specs=pl.BlockSpec(memory_space=vmem),
        scratch_shapes=scratch,
        compiler_params=pltpu.CompilerParams(
            collective_id=0, has_side_effects=True, vmem_limit_bytes=62 * 1024 * 1024
        ),
        name="layer",
    )(*small, *large)


def solution(mesh):
    placed = (
        P("ep", None),
        P(),
        P("ep", "tp"),
        P("ep", "tp"),
        P("ep", "tp"),
        P("ep", "tp"),
        P("tp", None),
        P("tp", None),
        P("ep", "tp", None, None),
        P("ep", "tp"),
        P("tp"),
        P(None, "ep"),
        P("ep"),
        P("ep"),
        P(),
        P(),
        P("ep", None, "tp"),
        P("ep", None, "tp"),
        P("ep", "tp", None),
        P("tp"),
    )
    return jax.shard_map(
        functools.partial(shards, mesh.shape["ep"], mesh.shape["tp"]),
        mesh=mesh, in_specs=placed, out_specs=P("ep", "tp"), check_vma=False,
    )
```

```python
import functools

import jax
import jax.numpy as jnp
from jax import lax
from jax.experimental import pallas as pl
from jax.experimental.pallas import tpu as pltpu
from jax.sharding import PartitionSpec as P

NORM_EPS = 1e-06
CLAMP_LIMIT = 7.0
SIGMOID_SCALE = 1.702
F32 = jnp.float32
BF16 = jnp.bfloat16


def rms_scale(values):
    return lax.rsqrt(jnp.mean(values * values, axis=-1, keepdims=True) + NORM_EPS)


def log_sigmoid(values):
    return jnp.minimum(values, 0.0) - jnp.log(1.0 + jnp.exp(-jnp.abs(values)))


def layer_kernel(n_ep, n_tp, *refs):
    (
        tokens, mixer_gain, igate, fgate, stabilizer, head_gain, mixed_gain, expert_gain,
        routes, route_weights, output_gain,
        query_weight, key_weight, value_weight, outgate_weight, memory, down_weight,
        gate_proj, up_proj, expert_down,
        out,
        w4, memv, downv, gatev, upv, edownv,
        xsend, xrecv, tok_all, gains, qk_send, qk_recv, vo_send, vo_recv, gsend, grecv, mixed_all, resid, expert_in,
        esend, apart, erecv, ssend, srecv, squares, read_rows,
        lsem, x_s, x_r, t_s, t_r, n_s, n_r, k_s, k_r, p_s, p_r, tf_s, tf_r, g_s, g_r, m_s, m_r, f_s, f_r,
        a_s, a_r, e_s, e_r, c_s, c_r, q_s, q_r,
    ) = refs
    me_e = lax.axis_index("ep")
    me_t = lax.axis_index("tp")
    rows, width = tokens.shape
    heads, head_size = memory.shape[1], memory.shape[3]
    head_width = heads * head_size
    slice_width = width // n_ep
    tp_width = width // n_tp
    ratio = n_ep // n_tp
    total = n_ep * rows
    quarter = ratio * rows
    experts = gate_proj.shape[0]

    def remote(src, dst, ssem, rsem, ep, tp):
        return pltpu.make_async_remote_copy(
            src_ref=src, dst_ref=dst, send_sem=ssem, recv_sem=rsem,
            device_id=(ep, tp), device_id_type=pl.DeviceIdType.MESH,
        )

    def loop(low, high, step):
        def run(i, carry):
            step(i)
            return carry

        lax.fori_loop(low, high, run, 0)

    def ep_at(i):
        return lax.rem(me_e + i, n_ep)

    def ep_back(i):
        return lax.rem(me_e - i + n_ep, n_ep)

    def tp_at(i):
        return lax.rem(me_t + i, n_tp)

    partner = me_t + 1 - 2 * lax.rem(me_t, 2)
    kin = [tp_at(i) for i in range(2, n_tp, 2)]
    strangers = [tp_at(i) for i in range(1, n_tp, 2)]

    local = []

    def fetch(src, dst):
        copy = pltpu.make_async_copy(src, dst, lsem.at[len(local)])
        copy.start()
        local.append(copy)
        return copy

    weight_copies = [
        fetch(ref, w4.at[i])
        for i, ref in enumerate((query_weight, key_weight, value_weight, outgate_weight))
    ]
    chunk = rows // 4
    memory_copies = [
        fetch(memory.at[pl.ds(i * chunk, chunk)], memv.at[pl.ds(i * chunk, chunk)])
        for i in range(4)
    ]
    down_copy = fetch(down_weight, downv)
    gate_copy = fetch(gate_proj, gatev)
    up_copy = fetch(up_proj, upv)
    edown_copy = fetch(expert_down, edownv)

    barrier = pltpu.get_barrier_semaphore()
    devices = n_ep * n_tp
    flat = me_e * n_tp + me_t

    def greet(i):
        other = lax.rem(flat + i, devices)
        pl.semaphore_signal(
            barrier, inc=1, device_id=(lax.div(other, n_tp), lax.rem(other, n_tp)),
            device_id_type=pl.DeviceIdType.MESH,
        )

    loop(1, devices, greet)

    tokens_float = tokens[...].astype(F32)
    normed = (tokens_float * rms_scale(tokens_float) * mixer_gain[...]).astype(BF16)
    for j in range(n_ep):
        xsend[j] = normed[:, j * slice_width : (j + 1) * slice_width]
    xrecv[me_e] = xsend[me_e]
    own_rows = pl.ds(pl.multiple_of(me_e * rows, rows), rows)
    tok_all[me_t, own_rows, :] = tokens[:, pl.ds(pl.multiple_of(me_t * tp_width, tp_width), tp_width)]
    gain_row = lax.broadcasted_iota(jnp.int32, (8, slice_width), 0)
    gains[me_e] = jnp.where(gain_row == 0, mixed_gain[...], expert_gain[...])
    pl.semaphore_wait(barrier, devices - 1)

    def x_copy(i):
        dst = ep_at(i)
        return remote(xsend.at[dst], xrecv.at[me_e], x_s.at[dst], x_r.at[me_e], dst, me_t)

    def t_copy(i):
        dst = ep_at(i)
        block = tok_all.at[me_t, own_rows]
        return remote(block, block, t_s.at[dst], t_r.at[me_e], dst, me_t)

    def n_copy(i):
        dst = ep_at(i)
        return remote(gains.at[me_e], gains.at[me_e], n_s.at[dst], n_r.at[me_e], dst, me_t)

    loop(1, n_ep, lambda i: x_copy(i).start())

    normed_float = normed.astype(F32)
    log_input = [
        jnp.sum(normed_float * igate[h : h + 1, :].astype(F32), axis=-1, keepdims=True)
        for h in range(heads)
    ]
    log_forget = [
        log_sigmoid(jnp.sum(normed_float * fgate[h : h + 1, :].astype(F32), axis=-1, keepdims=True))
        for h in range(heads)
    ]

    for copy in weight_copies:
        copy.wait()

    def x_wait(i):
        src = ep_back(i)
        remote(xrecv.at[src], xrecv.at[src], x_s.at[src], x_r.at[src], src, me_t).wait_recv()

    loop(1, n_ep, x_wait)
    features = jnp.concatenate([xrecv[j] for j in range(n_ep)], axis=0)

    def k_copy(j, i):
        dst = ep_at(i)
        return remote(
            qk_send.at[j, dst], qk_recv.at[j, me_e], k_s.at[j, dst], k_r.at[j, me_e], dst, me_t
        )

    def p_copy(i):
        dst = ep_at(i)
        return remote(vo_send.at[dst], vo_recv.at[me_e], p_s.at[dst], p_r.at[me_e], dst, me_t)

    for j in range(2):
        part = jnp.dot(features, w4[j], preferred_element_type=F32)
        qk_send[j] = part.reshape(n_ep, rows, head_width)
        loop(1, n_ep, lambda i: k_copy(j, i).start())
        qk_recv[j, me_e] = qk_send[j, me_e]
        if j == 0:
            loop(1, n_ep, lambda i: t_copy(i).start())
    for j in range(2):
        part = jnp.dot(features, w4[2 + j], preferred_element_type=F32).astype(BF16)
        vo_send[:, :, j * head_width : (j + 1) * head_width] = part.reshape(n_ep, rows, head_width)
    loop(1, n_ep, lambda i: p_copy(i).start())
    vo_recv[me_e] = vo_send[me_e]
    loop(1, n_ep, lambda i: n_copy(i).start())

    def k_wait(j, i):
        src = ep_back(i)
        block = qk_recv.at[j, src]
        remote(block, block, k_s.at[j, src], k_r.at[j, src], src, me_t).wait_recv()

    def p_wait(i):
        src = ep_back(i)
        remote(vo_recv.at[src], vo_recv.at[src], p_s.at[src], p_r.at[src], src, me_t).wait_recv()

    def total_of(ref, *lead):
        value = ref[(*lead, 0)].astype(F32)
        for j in range(1, n_ep):
            value = value + ref[(*lead, j)].astype(F32)
        return value.astype(BF16).astype(F32)

    loop(1, n_ep, lambda i: k_wait(0, i))

    def t_wait(i):
        src = ep_back(i)
        block = tok_all.at[me_t, pl.ds(pl.multiple_of(src * rows, rows), rows)]
        remote(block, block, t_s.at[src], t_r.at[src], src, me_t).wait_recv()

    loop(1, n_ep, t_wait)

    def tf_copy(t, dst, slot):
        return remote(tok_all.at[t], tok_all.at[t], tf_s.at[slot], tf_r.at[t], me_e, dst)

    for t in kin + [partner]:
        tf_copy(me_t, t, t).start()
    all_query = total_of(qk_recv, 0) * head_size ** (-0.5)

    for copy in memory_copies:
        copy.wait()
    for h in range(heads):
        query_columns = all_query[:, h * head_size : (h + 1) * head_size].T
        for n in range(rows):
            column = query_columns[:, n : n + 1]
            step = 64
            acc = jnp.zeros((8, head_size), F32)
            for d in range(0, head_size, step):
                prod = column[d : d + step, :] * memv[n, h, d : d + step, :]
                acc = acc + jnp.sum(prod.reshape(step // 8, 8, head_size), axis=0)
            read_rows[h, n : n + 1, :] = jnp.sum(acc, axis=0, keepdims=True)
    loop(1, n_ep, lambda i: k_wait(1, i))
    all_key = total_of(qk_recv, 1)
    loop(1, n_ep, p_wait)
    all_gated = total_of(vo_recv)
    for h in range(heads):
        head = slice(h * head_size, (h + 1) * head_size)
        query, key = all_query[:, head], all_key[:, head]
        value = all_gated[:, head]
        outgate = all_gated[:, head_width + h * head_size : head_width + (h + 1) * head_size]
        carried_log = log_forget[h] + stabilizer[:, h : h + 1]
        peak = jnp.maximum(carried_log, log_input[h])
        within = jnp.exp(log_input[h] - peak)
        carried = jnp.exp(carried_log - peak)
        score = jnp.sum(query * key, axis=-1, keepdims=True) * within
        read = score * value + carried * read_rows[h]
        centered = read - jnp.mean(read, axis=-1, keepdims=True)
        variance = jnp.mean(centered * centered, axis=-1, keepdims=True)
        gained = centered * lax.rsqrt(variance + NORM_EPS)
        gained = gained * head_gain[:, h * head_size : (h + 1) * head_size]
        gained = gained * jax.nn.sigmoid(outgate)
        gsend[:, h * head_size : (h + 1) * head_size] = gained.astype(BF16)

    group = lax.div(me_e, ratio)
    place = lax.rem(me_e, ratio)
    place_rows = pl.ds(pl.multiple_of(place * rows, rows), rows)
    home = group == me_t

    def g_copy(dst):
        return remote(
            gsend, grecv.at[me_t, place_rows], g_s.at[dst], g_r.at[place * n_tp + me_t], dst, group
        )

    @pl.when(home)
    def _():
        grecv[me_t, place_rows, :] = gsend[...]

    @pl.when(jnp.logical_not(home))
    def _():
        g_copy(me_e).start()

    loop(1, n_ep, lambda i: g_copy(ep_at(i)).start())

    for t in kin:
        remote(tok_all.at[t], tok_all.at[t], tf_s.at[t], tf_r.at[t], me_e, t).wait_recv()
        tf_copy(t, partner, n_tp + t).start()

    def g_wait(k):
        src_place, src_t = lax.div(k, n_tp), lax.rem(k, n_tp)
        src_e = me_t * ratio + src_place

        @pl.when(jnp.logical_or(src_e != me_e, src_t != me_t))
        def _():
            block = grecv.at[src_t, pl.ds(pl.multiple_of(src_place * rows, rows), rows)]
            remote(block, block, g_s.at[0], g_r.at[k], src_e, src_t).wait_recv()

    down_copy.wait()
    loop(0, ratio * n_tp, g_wait)
    mixed = jnp.dot(grecv[0], downv[0:head_width, :], preferred_element_type=F32)
    for s in range(1, n_tp):
        mixed = mixed + jnp.dot(
            grecv[s], downv[s * head_width : (s + 1) * head_width, :], preferred_element_type=F32
        )

    def token_rows(t):
        return pl.ds(pl.multiple_of(t * quarter, quarter), quarter)

    mixed_all[me_e, token_rows(me_t), :] = mixed.astype(BF16)

    def m_copy(i):
        dst = ep_at(i)
        block = mixed_all.at[me_e, token_rows(me_t)]
        return remote(block, block, m_s.at[dst], m_r.at[me_e], dst, me_t)

    def f_copy(src, t, dst, slot):
        block = mixed_all.at[src, token_rows(t)]
        return remote(block, block, f_s.at[src, slot], f_r.at[src, t], me_e, dst)

    def f_wait(src, t):
        f_copy(src, t, t, t).wait_recv()

    def f_spread(src):
        for t in kin + [partner]:
            f_copy(src, me_t, t, t).start()

    def f_pass(i):
        src = ep_back(i)
        for t in kin:
            f_wait(src, t)
            f_copy(src, t, partner, n_tp + t).start()

    loop(1, n_ep, lambda i: m_copy(i).start())
    f_spread(me_e)

    def m_pass(i):
        src = ep_back(i)
        block = mixed_all.at[src, token_rows(me_t)]
        remote(block, block, m_s.at[src], m_r.at[src], src, me_t).wait_recv()
        f_spread(src)

    loop(1, n_ep, m_pass)
    loop(0, n_ep, f_pass)

    def n_wait(i):
        src = ep_back(i)
        remote(gains.at[src], gains.at[src], n_s.at[src], n_r.at[src], src, me_t).wait_recv()

    loop(1, n_ep, n_wait)
    for t in strangers:
        remote(tok_all.at[t], tok_all.at[t], tf_s.at[t], tf_r.at[t], me_e, t).wait_recv()

    def f_rest(i):
        for t in strangers:
            f_wait(ep_back(i), t)

    loop(0, n_ep, f_rest)

    mixed_squares = jnp.zeros((total, 1), F32)
    for j in range(n_ep):
        block = mixed_all[j].astype(F32)
        mixed_squares = mixed_squares + jnp.sum(block * block, axis=-1, keepdims=True)
    mixed_scale = lax.rsqrt(mixed_squares / width + NORM_EPS)
    residual_squares = jnp.zeros((total, 1), F32)
    for j in range(n_ep):
        start = j * slice_width
        owner, offset = start // tp_width, start % tp_width
        block = tok_all[owner, :, offset : offset + slice_width].astype(F32)
        block = block + mixed_all[j].astype(F32) * mixed_scale * gains[j, 0:1, :]
        resid[:, start : start + slice_width] = block
        residual_squares = residual_squares + jnp.sum(block * block, axis=-1, keepdims=True)
    residual_scale = lax.rsqrt(residual_squares / width + NORM_EPS)
    for j in range(n_ep):
        start = j * slice_width
        block = resid[:, start : start + slice_width] * residual_scale * gains[j, 1:2, :]
        expert_in[:, start : start + slice_width] = block.astype(BF16)

    gate_copy.wait()
    up_copy.wait()
    acts, weights = [], []
    for l in range(experts):
        gate = jnp.dot(expert_in[...], gatev[l], preferred_element_type=F32)
        up = jnp.dot(expert_in[...], upv[l], preferred_element_type=F32)
        gate = jnp.minimum(gate, CLAMP_LIMIT)
        up = jnp.clip(up, -CLAMP_LIMIT, CLAMP_LIMIT)
        acts.append(((up + 1.0) * gate * jax.nn.sigmoid(SIGMOID_SCALE * gate)).astype(BF16))
        hit = routes[...] == me_e * experts + l
        weights.append(jnp.sum(jnp.where(hit, route_weights[...], 0.0), axis=-1, keepdims=True))
    edown_copy.wait()

    def expert_part(t):
        columns = pl.ds(pl.multiple_of(t * tp_width, tp_width), tp_width)
        value = None
        for l in range(experts):
            one = jnp.dot(acts[l], edownv[l, :, columns], preferred_element_type=F32) * weights[l]
            value = one if value is None else value + one
        return value

    def a_copy(i, t):
        return remote(esend.at[i], apart.at[t], a_s.at[i], a_r.at[t], me_e, partner)

    def a_part(t):
        remote(apart.at[t], apart.at[t], a_s.at[0], a_r.at[t], me_e, partner).wait_recv()
        return apart[t].astype(F32)

    def e_copy(i, t):
        return remote(esend.at[half + i], erecv.at[me_t], e_s.at[i], e_r.at[me_t], me_e, t)

    half = n_tp // 2
    pair_order = [lax.rem(partner + i, n_tp) for i in range(2, n_tp, 2)] + [partner]
    for i, t in enumerate(pair_order):
        esend[i] = expert_part(t).astype(BF16)
        a_copy(i, t).start()
    for i, t in enumerate(kin):
        own_part = expert_part(t)
        esend[half + i] = (own_part + a_part(t)).astype(BF16)
        e_copy(i, t).start()
    combined_part = expert_part(me_t)
    combined_part = combined_part + a_part(me_t)
    for t in kin:
        remote(erecv.at[t], erecv.at[t], e_s.at[0], e_r.at[t], me_e, t).wait_recv()
        combined_part = combined_part + erecv[t].astype(F32)
    ssend[...] = combined_part.astype(BF16).reshape(n_ep, rows, tp_width)

    def c_copy(i):
        dst = ep_at(i)
        return remote(ssend.at[dst], srecv.at[me_e], c_s.at[dst], c_r.at[me_e], dst, me_t)

    loop(1, n_ep, lambda i: c_copy(i).start())
    srecv[me_e] = ssend[me_e]

    def c_wait(i):
        src = ep_back(i)
        remote(srecv.at[src], srecv.at[src], c_s.at[src], c_r.at[src], src, me_t).wait_recv()

    loop(1, n_ep, c_wait)
    combined = srecv[0].astype(F32)
    for j in range(1, n_ep):
        combined = combined + srecv[j].astype(F32)
    own_squares = jnp.sum(combined * combined, axis=-1, keepdims=True)
    squares[me_t] = jnp.broadcast_to(own_squares, squares.shape[1:])

    def q_copy(i):
        dst = tp_at(i)
        return remote(squares.at[me_t], squares.at[me_t], q_s.at[dst], q_r.at[me_t], me_e, dst)

    loop(1, n_tp, lambda i: q_copy(i).start())
    own_columns = pl.ds(pl.multiple_of(me_t * tp_width, tp_width), tp_width)
    residual = resid[own_rows, own_columns].astype(BF16).astype(F32)

    def q_wait(i):
        src = tp_at(i)
        remote(squares.at[src], squares.at[src], q_s.at[src], q_r.at[src], me_e, src).wait_recv()

    loop(1, n_tp, q_wait)
    all_squares = squares[0]
    for t in range(1, n_tp):
        all_squares = all_squares + squares[t]
    scale = lax.rsqrt(all_squares[:, 0:1] / width + NORM_EPS)
    out[...] = (residual + combined * scale * output_gain[...]).astype(BF16)

    def ep_sends(i):
        x_copy(i).wait_send()
        t_copy(i).wait_send()
        n_copy(i).wait_send()
        k_copy(0, i).wait_send()
        k_copy(1, i).wait_send()
        p_copy(i).wait_send()
        g_copy(ep_at(i)).wait_send()
        m_copy(i).wait_send()
        c_copy(i).wait_send()

    loop(1, n_ep, ep_sends)

    @pl.when(jnp.logical_not(home))
    def _():
        g_copy(me_e).wait_send()

    loop(1, n_tp, lambda i: q_copy(i).wait_send())
    for t in kin + [partner]:
        tf_copy(me_t, t, t).wait_send()
    for t in kin:
        tf_copy(t, partner, n_tp + t).wait_send()
    for i, t in enumerate(pair_order):
        a_copy(i, t).wait_send()
    for i, t in enumerate(kin):
        e_copy(i, t).wait_send()

    def f_sends(i):
        src = ep_back(i)
        for t in kin + [partner]:
            f_copy(src, me_t, t, t).wait_send()
        for t in kin:
            f_copy(src, t, partner, n_tp + t).wait_send()

    loop(0, n_ep, f_sends)


def shards(
    n_ep, n_tp, tokens, mixer_gain, query_weight, key_weight, value_weight, outgate_weight,
    igate_weight, fgate_weight, memory, stabilizer, head_gain, down_weight, mixed_gain,
    expert_gain, routes, route_weights, gate_proj, up_proj, expert_down, output_gain,
):
    rows, width = tokens.shape
    heads, head_size = memory.shape[1], memory.shape[3]
    head_width = heads * head_size
    slice_width = width // n_ep
    tp_width = width // n_tp
    total = n_ep * rows
    quarter = total // n_tp
    vmem = pltpu.VMEM
    dma = pltpu.SemaphoreType.DMA
    small = (
        tokens, mixer_gain.reshape(1, -1), igate_weight, fgate_weight, stabilizer,
        head_gain.reshape(1, -1), mixed_gain.reshape(1, -1), expert_gain.reshape(1, -1),
        routes, route_weights, output_gain.reshape(1, -1),
    )
    large = (
        query_weight, key_weight, value_weight, outgate_weight, memory, down_weight,
        gate_proj, up_proj, expert_down,
    )
    scratch = [
        vmem((4,) + query_weight.shape, BF16),
        vmem(memory.shape, F32),
        vmem(down_weight.shape, BF16),
        vmem(gate_proj.shape, BF16),
        vmem(up_proj.shape, BF16),
        vmem(expert_down.shape, BF16),
        vmem((n_ep, rows, slice_width), BF16),
        vmem((n_ep, rows, slice_width), BF16),
        vmem((n_tp, total, tp_width), BF16),
        vmem((n_ep, 8, slice_width), F32),
        vmem((2, n_ep, rows, head_width), F32),
        vmem((2, n_ep, rows, head_width), F32),
        vmem((n_ep, rows, 2 * head_width), BF16),
        vmem((n_ep, rows, 2 * head_width), BF16),
        vmem((rows, head_width), BF16),
        vmem((n_tp, quarter, head_width), BF16),
        vmem((n_ep, total, slice_width), BF16),
        vmem((total, width), F32),
        vmem((total, width), BF16),
        vmem((n_tp, total, tp_width), BF16),
        vmem((n_tp, total, tp_width), BF16),
        vmem((n_tp, total, tp_width), BF16),
        vmem((n_ep, rows, tp_width), BF16),
        vmem((n_ep, rows, tp_width), BF16),
        vmem((n_tp, rows, 128), F32),
        vmem((heads, rows, head_size), F32),
        dma((12,)),
        dma((n_ep,)), dma((n_ep,)),
        dma((n_ep,)), dma((n_ep,)),
        dma((n_ep,)), dma((n_ep,)),
        dma((2, n_ep)), dma((2, n_ep)),
        dma((n_ep,)), dma((n_ep,)),
        dma((2 * n_tp,)), dma((n_tp,)),
        dma((n_ep,)), dma((n_ep,)),
        dma((n_ep,)), dma((n_ep,)),
        dma((n_ep, 2 * n_tp)), dma((n_ep, n_tp)),
        dma((n_tp,)), dma((n_tp,)),
        dma((n_tp,)), dma((n_tp,)),
        dma((n_ep,)), dma((n_ep,)),
        dma((n_tp,)), dma((n_tp,)),
    ]
    return pl.pallas_call(
        functools.partial(layer_kernel, n_ep, n_tp),
        out_shape=jax.ShapeDtypeStruct((rows, tp_width), BF16),
        in_specs=[pl.BlockSpec(memory_space=vmem)] * len(small)
        + [pl.BlockSpec(memory_space=pl.ANY)] * len(large),
        out_specs=pl.BlockSpec(memory_space=vmem),
        scratch_shapes=scratch,
        compiler_params=pltpu.CompilerParams(
            collective_id=0, has_side_effects=True, vmem_limit_bytes=62 * 1024 * 1024
        ),
        name="layer",
    )(*small, *large)


def solution(mesh):
    placed = (
        P("ep", None),
        P(),
        P("ep", "tp"),
        P("ep", "tp"),
        P("ep", "tp"),
        P("ep", "tp"),
        P("tp", None),
        P("tp", None),
        P("ep", "tp", None, None),
        P("ep", "tp"),
        P("tp"),
        P(None, "ep"),
        P("ep"),
        P("ep"),
        P(),
        P(),
        P("ep", None, "tp"),
        P("ep", None, "tp"),
        P("ep", "tp", None),
        P("tp"),
    )
    return jax.shard_map(
        functools.partial(shards, mesh.shape["ep"], mesh.shape["tp"]),
        mesh=mesh, in_specs=placed, out_specs=P("ep", "tp"), check_vma=False,
    )
```
